256 devices in a mesh: fs: 64 (over z, y, core), tp: 4 (over x).
Axes of the slice: x: 4, y: 4, z: 8, core: 2. Of those that a mesh axis runs over, the one named last changes fastest.
Arguments:
- later_gate: bfloat16 [40960, 5632], P('fs', 'tp'), may hold values from -6 to 6
- later_up: bfloat16 [40960, 5632], P('fs', 'tp'), may hold values from -6 to 6
- early_gate: bfloat16 [40960, 5632], P('fs', 'tp'), may hold values from -6 to 6
- early_up: bfloat16 [40960, 5632], P('fs', 'tp'), may hold values from -6 to 6
- early_cotangent: bfloat16 [40960, 2048], P(('fs', 'tp')), may hold values from -24 to 24
- down_weight: bfloat16 [5632, 2048], P('tp', 'fs'), may hold values from -0.078125 to 0.078125
- grad_running: float32 [5632, 2048], P('tp', 'fs'), may hold values from -640 to 640
Outputs:
- mixed: bfloat16 [40960, 2048], P(('fs', 'tp'))
- gate_grad: bfloat16 [40960, 5632], P('fs', 'tp')
- up_grad: bfloat16 [40960, 5632], P('fs', 'tp')
- grad_total: float32 [5632, 2048], P('tp', 'fs')
The draws below stay inside these ranges and needn't reach their ends.
All inputs are finite; a program needn't handle non-finite values.
Results may differ from the reference program's by a relative error of at most 0.009.
Values may be sent and summed in bfloat16 or wider, within the bound.
A program may use at most 128 MiB of HBM per device.

```python
import jax
import jax.numpy as jnp

D = 2048
FF = 5632
TOKENS = 40960
N_TP = 4


def raised(entries, own_key, source, target, shards_of, factor):
    owner, partner = [(jnp.arange(entries.shape[dim]) // (entries.shape[dim] // shards_of)).reshape([-1 if axis == dim else 1 for axis in range(entries.ndim)]) for dim in (source, target)]
    chosen = jax.random.permutation(own_key, shards_of)[partner]
    strong = (owner == chosen) | (owner == (partner + shards_of // 2) % shards_of)
    return jnp.where(strong, factor * entries, entries)


def steps_of(rng, extent, pieces, least, top_value):
    factor_of, own = 1.0, jax.random.fold_in(rng, 6)
    for axis_at, shards_of in pieces:
        steps = jnp.exp(jax.random.uniform(jax.random.fold_in(own, axis_at), (shards_of,), jnp.float32, least / len(pieces), top_value / len(pieces)))
        factor_of = factor_of * jnp.repeat(steps, extent[axis_at] // shards_of).reshape([-1 if axis == axis_at else 1 for axis in range(len(extent))])
    return factor_of


def centred(rng, shape, width, reach, shards=(), kind=jnp.bfloat16):
    values = jax.random.normal(rng, shape, jnp.float32) * width
    if len(shards) > 0:
        values = steps_of(rng, shape, shards, -0.22, 0.18) * values
    return jnp.clip(values, min=-reach, max=reach).astype(kind)


def bell_draw_with(own_key, shape, spread, most, cuts, heavy, dtype=jnp.bfloat16):
    drawn = spread * jax.random.normal(own_key, shape, jnp.float32)
    if cuts:
        drawn = drawn * steps_of(own_key, shape, cuts, -0.22, 0.18)
    return jnp.clip(raised(drawn, jax.random.fold_in(own_key, 3), *heavy), -most, most).astype(dtype)


def setup_inputs(seed: int = 0) -> dict:
    key_list = jax.random.split(jax.random.key(seed), 8)
    return {
        "later_gate": centred(key_list[0], (TOKENS, FF), 1.0, 6.0, ((0, 64), (1, 4))),
        "later_up": centred(key_list[1], (TOKENS, FF), 1.0, 6.0, ((0, 64), (1, 4))),
        "early_gate": centred(key_list[2], (TOKENS, FF), 1.0, 6.0, ((0, 64), (1, 4))),
        "early_up": centred(key_list[3], (TOKENS, FF), 1.0, 6.0, ((0, 64), (1, 4))),
        "early_cotangent": bell_draw_with(key_list[4], (TOKENS, D), 1.0, 24.0, ((0, 256),), (0, 1, 256, 6.0)),
        "down_weight": centred(key_list[5], (FF, D), FF ** -0.5, 0.078125, ((0, 4), (1, 64))),
        "grad_running": centred(key_list[6], (FF, D), (0.5 * TOKENS ** 0.5), 640.0, ((0, 4), (1, 64)), jnp.float32),
    }


def reference(later_gate, later_up, early_gate, early_up, early_cotangent, down_weight, grad_running):
    later_hidden = (jax.nn.silu(later_gate.astype(jnp.float32)) * later_up.astype(jnp.float32)).astype(jnp.bfloat16)
    block = FF // N_TP
    total = jnp.zeros((later_hidden.shape[0], D), jnp.float32)
    for index in range(N_TP):
        part = jnp.dot(later_hidden[:, index * block:(index + 1) * block], down_weight[index * block:(index + 1) * block], preferred_element_type=jnp.float32)
        total = total + part.astype(jnp.bfloat16).astype(jnp.float32)
    mixed = total.astype(jnp.bfloat16)
    gate_value = early_gate.astype(jnp.float32)
    up_value = early_up.astype(jnp.float32)
    sigma = jax.nn.sigmoid(gate_value)
    early_hidden = (gate_value * sigma * up_value).astype(jnp.bfloat16)
    hidden_cot = jnp.dot(early_cotangent, down_weight.T, preferred_element_type=jnp.float32)
    gate_grad = (hidden_cot * up_value * sigma * (1.0 + gate_value * (1.0 - sigma))).astype(jnp.bfloat16)
    up_grad = (hidden_cot * gate_value * sigma).astype(jnp.bfloat16)
    grad_total = grad_running + jnp.dot(early_hidden.T, early_cotangent, preferred_element_type=jnp.float32)
    return (mixed, gate_grad, up_grad, grad_total)
```

```python
import functools

import jax
import jax.numpy as jnp
from jax import lax
from jax.experimental import pallas as pl
from jax.experimental.pallas import tpu as pltpu
from jax.sharding import PartitionSpec as P

MESH = pl.DeviceIdType.MESH
F32, BF16 = jnp.float32, jnp.bfloat16
NX, NY, NZ, NC = 4, 4, 8, 2
ROWS = 32
WIDE = NY * NC * ROWS
TILE = 16


def sigmoid(v):
    return 0.5 * jnp.tanh(0.5 * v) + 0.5


def kernel(
    lg_h, lu_h, eg_h, eu_h, cot_h, wt_h,
    mixed_o, gg_o, ug_o, gsum_o,
    lg, lu, eg, eu, eh, cot, wt, gbuf, precv, zrecv, yrecv, pbuf, pre, full, mixed, hc, gsum,
    load_sem, out_sem,
    cd_s, cd_r, cf_s, cf_r,
    wz_s, wz_r, wy_s, wy_r, wf_s, wf_r, wd_s, wd_r,
    gp_s, gp_r, gz_s, gz_r, gy_s, gy_r,
    mp_s, mp_r, mf_s, mf_r,
):
    f, x = lax.axis_index("fs"), lax.axis_index("tp")
    c, y, z = lax.rem(f, NC), lax.rem(f // NC, NY), f // (NC * NY)
    xrows = cot_h.shape[0]
    half = xrows // 2
    hrow = ROWS // 2
    tokens = NX * xrows

    def dx(k):
        return lax.rem(x + (k + NX), NX)

    def dy(k):
        return lax.rem(y + (k + NY), NY)

    def dz(k):
        return lax.rem(z + (k + NZ), NZ)

    def at_x(k):
        return (f, dx(k))

    def at_y(k):
        return ((z * NY + dy(k)) * NC + c, x)

    def at_z(k):
        return ((dz(k) * NY + y) * NC + c, x)

    partner = ((z * NY + y) * NC + (1 - c), x)

    sends, outs = [], []

    def send(src, dst, ssem, rsem, to):
        copy = pltpu.make_async_remote_copy(
            src_ref=src, dst_ref=dst, send_sem=ssem, recv_sem=rsem, device_id=to, device_id_type=MESH
        )
        copy.start()
        sends.append(copy)

    def arrived(dst, ssem, rsem):
        pltpu.make_async_remote_copy(
            src_ref=dst, dst_ref=dst, send_sem=ssem, recv_sem=rsem, device_id=partner, device_id_type=MESH
        ).wait_recv()

    loads = [
        pltpu.make_async_copy(src, dst, load_sem.at[i])
        for i, (src, dst) in enumerate(
            [
                (eg_h, eg),
                (eu_h, eu),
                (cot_h, cot.at[pl.ds(pl.multiple_of(x * xrows, TILE), xrows)]),
                (wt_h, wt.at[z * NY + y, c]),
                (lg_h, lg),
                (lu_h, lu),
            ]
        )
    ]
    for copy in loads:
        copy.start()

    barrier = pltpu.get_barrier_semaphore()
    peers = [at_x(1), at_x(-1), at_y(1), at_y(-1), at_y(2), at_z(1), at_z(-1), partner]
    for peer in peers:
        pl.semaphore_signal(barrier, inc=1, device_id=peer, device_id_type=MESH)
    pl.semaphore_wait(barrier, len(peers))

    SIDES = ((0, 1), (1, -1))
    ZSTEPS = (4, 3, -3, 2, -2, 1, -1, 0)
    WSTEPS = (0, -1, 1, -2, 2, -3, 3, 4)

    def columns(step):
        return pl.ds(pl.multiple_of(dz(step) * WIDE, WIDE), WIDE)

    def cot_rows(step, start=0, size=xrows):
        return pl.ds(pl.multiple_of(dx(step) * xrows + start, TILE), size)

    def cot_direct(k):
        cols = columns(ZSTEPS[k])
        for d, s in SIDES:
            send(cot_h.at[:, cols], cot.at[cot_rows(0), cols], cd_s.at[d, k], cd_r.at[d, k], at_x(s))

    def cot_forward(k):
        cols = columns(ZSTEPS[k])
        for d, s in SIDES:
            block = cot.at[cot_rows(-s), cols]
            arrived(block, cd_s.at[d, k], cd_r.at[d, k])
            part = cot.at[cot_rows(-s, d * half, half), cols]
            send(part, part, cf_s.at[d, k], cf_r.at[d, k], at_x(s))
        if k + 2 < NZ:
            cot_direct(k + 2)

    def cot_done(k):
        cols = columns(ZSTEPS[k])
        for d, s in SIDES:
            part = cot.at[cot_rows(2, d * half, half), cols]
            arrived(part, cf_s.at[d, k], cf_r.at[d, k])

    def w_block(zs, ys):
        return wt.at[dz(zs) * NY + dy(ys), c]

    def w_along_z(s):
        for d, step in SIDES:
            block = w_block(-step * (s - 1), 0)
            if s == 4:
                block = block.at[pl.ds(d * hrow, hrow)]
            send(block, block, wz_s.at[d, s - 1], wz_r.at[d, s - 1], at_z(step))

    def w_along_y(j):
        block = w_block(WSTEPS[j], 0)
        for d, step in SIDES:
            send(block, block, wy_s.at[d, j], wy_r.at[d, j], at_y(step))

    def w_z(s):
        for d, step in SIDES:
            block = w_block(-step * s, 0)
            if s == 4:
                block = block.at[pl.ds(d * hrow, hrow)]
            arrived(block, wz_s.at[d, s - 1], wz_r.at[d, s - 1])
        if s < 4:
            w_along_z(s + 1)
            w_along_y(2 * s - 1)
            w_along_y(2 * s)
        else:
            w_along_y(7)

    def w_y(j):
        for d, step in SIDES:
            block = w_block(WSTEPS[j], -step)
            arrived(block, wy_s.at[d, j], wy_r.at[d, j])
            part = block.at[pl.ds(d * hrow, hrow)]
            send(part, part, wf_s.at[d, j], wf_r.at[d, j], at_y(step))

    def w_core(j):
        for d, step in SIDES:
            part = w_block(WSTEPS[j], 2).at[pl.ds(d * hrow, hrow)]
            arrived(part, wf_s.at[d, j], wf_r.at[d, j])
        rows = wt.at[pl.ds(dz(WSTEPS[j]) * NY, NY), c]
        send(rows, rows, wd_s.at[j], wd_r.at[j], partner)

    def w_done(j):
        rows = wt.at[pl.ds(dz(WSTEPS[j]) * NY, NY), 1 - c]
        arrived(rows, wd_s.at[j], wd_r.at[j])

    def over_rows(first, size, body):
        def step(i, carry):
            body(pl.ds(pl.multiple_of(first + i * TILE, TILE), TILE))
            return carry

        lax.fori_loop(0, size // TILE, step, 0)

    def early(first, size):
        def body(rows):
            gate = eg[rows, :].astype(F32)
            eh[rows, :] = (gate * sigmoid(gate) * eu[rows, :].astype(F32)).astype(BF16)

        over_rows(first, size, body)

    def later(first, size):
        def body(rows):
            gate = lg[rows, :].astype(F32)
            lg[rows, :] = (gate * sigmoid(gate) * lu[rows, :].astype(F32)).astype(BF16)

        over_rows(first, size, body)

    def grad(k):
        cot_done(k)
        part = lax.dot_general(
            cot[:, columns(ZSTEPS[k])], eh[...], (((0,), (0,)), ((), ())), preferred_element_type=F32
        )
        gbuf[k] = part.astype(BF16).reshape(NY, NC, ROWS, part.shape[1])
        send(gbuf.at[k, :, 1 - c], precv.at[k], gp_s.at[k], gp_r.at[k], partner)

    def pair_done(k):
        arrived(precv.at[k], gp_s.at[k], gp_r.at[k])

    def add_up(k, h, more):
        def step(i, carry):
            r, rows = i // 2, pl.ds(pl.multiple_of(lax.rem(i, 2) * TILE, TILE), TILE)
            total = gbuf[k, 2 * h + r, c, rows].astype(F32)
            total += precv[k, 2 * h + r, rows].astype(F32)
            for d, i_at in more:
                total += zrecv[d, i_at, r, rows].astype(F32)
            gbuf[k, 2 * h + r, c, rows] = total.astype(BF16)
            return carry

        lax.fori_loop(0, 4, step, 0)

    CHAIN = (
        ((0, 0), (1, 1), (1, 0), (3, 1), (3, 0), (5, 1), (5, 0)),
        ((0, 1), (2, 0), (2, 1), (4, 0), (4, 1), (6, 0), (6, 1)),
    )

    def chain_arrived(d, i):
        arrived(zrecv.at[d, i], gz_s.at[d, i], gz_r.at[d, i])

    def chain(d, i):
        k, h = CHAIN[d][i]
        if i >= 2:
            chain_arrived(d, i - 2)
        add_up(k, h, [(d, i - 2)] if i >= 2 else [])
        step = SIDES[d][1]
        send(gbuf.at[k, pl.ds(2 * h, 2), c], zrecv.at[d, i], gz_s.at[d, i], gz_r.at[d, i], at_z(step))

    def own_sum():
        for d in (0, 1):
            for i in (5, 6):
                chain_arrived(d, i)
        for h in (0, 1):
            add_up(7, h, [(0, 6 - h), (1, 5 + h)])
        for i, step in enumerate((1, -1, 2)):
            send(gbuf.at[7, dy(step), c], yrecv.at[i], gy_s.at[i], gy_r.at[i], at_y(step))

    def grad_end():
        for i in range(3):
            arrived(yrecv.at[i], gy_s.at[i], gy_r.at[i])
        total = gbuf[7, y, c].astype(F32)
        for i in range(3):
            total += yrecv[i].astype(F32)
        gsum[...] = total
        copy = pltpu.make_async_copy(gsum, gsum_o, out_sem.at[0])
        copy.start()
        outs.append(copy)

    def partial(j):
        w_done(j)
        rows = wt[pl.ds(dz(WSTEPS[j]) * NY, NY)].reshape(WIDE, wt.shape[3])
        part = lax.dot_general(lg[...], rows, (((1,), (1,)), ((), ())), preferred_element_type=F32)
        pbuf[j] = part.astype(BF16).reshape(NX, xrows, WIDE)
        for d, s in SIDES:
            send(pbuf.at[j, dx(2), pl.ds(d * half, half)], pre.at[d, j], mp_s.at[d, j], mp_r.at[d, j], at_x(s))

    def partial_on(j):
        for d, s in SIDES:
            arrived(pre.at[d, j], mp_s.at[d, j], mp_r.at[d, j])
            rows = pl.ds(d * half, half)
            pbuf[j, dx(s), rows] = (pbuf[j, dx(s), rows].astype(F32) + pre[d, j].astype(F32)).astype(BF16)
            send(pbuf.at[j, dx(s)], full.at[d, j], mf_s.at[d, j], mf_r.at[d, j], at_x(s))

    def partial_end(j):
        total = pbuf[j, x].astype(F32)
        for d, s in SIDES:
            arrived(full.at[d, j], mf_s.at[d, j], mf_r.at[d, j])
            total += full[d, j].astype(F32)
        cols = columns(WSTEPS[j])
        mixed[:, cols] = total.astype(BF16)
        copy = pltpu.make_async_copy(mixed.at[:, cols], mixed_o.at[:, cols], out_sem.at[1 + j])
        copy.start()
        outs.append(copy)

    def hidden(m):
        rows = pl.ds(m * xrows, xrows)
        hc[...] = jnp.dot(
            cot[rows, :], wt[...].reshape(NZ * WIDE, wt.shape[3]), preferred_element_type=F32
        )

    def pointwise(m):
        def body(rows):
            sub = pl.ds(rows.start - m * xrows, TILE)
            gate, up, cotan = eg[rows, :].astype(F32), eu[rows, :].astype(F32), hc[sub, :]
            s = sigmoid(gate)
            scaled = cotan * s
            eg[rows, :] = (scaled * up * (1.0 + gate * (1.0 - s))).astype(BF16)
            eu[rows, :] = (scaled * gate).astype(BF16)

        over_rows(m * xrows, xrows, body)
        rows = pl.ds(m * xrows, xrows)
        for i, (src, dst) in enumerate(((eg, gg_o), (eu, ug_o))):
            copy = pltpu.make_async_copy(src.at[rows], dst.at[rows], out_sem.at[9 + 2 * m + i])
            copy.start()
            outs.append(copy)

    tasks = []

    def at(time, run, *args):
        tasks.append((time, len(tasks), run, args))

    def begin():
        cot_direct(0)
        loads[3].wait()
        w_along_z(1)
        w_along_y(0)
        cot_direct(1)
        loads[0].wait()
        loads[1].wait()

    def later_loads():
        loads[4].wait()
        loads[5].wait()

    at(0, begin)
    quarter = tokens // 4
    for i in range(4):
        at(1.2 + 0.75 * i, early, i * quarter, quarter)
    at(3.9, loads[2].wait)
    at(6.0, later_loads)
    for i, t in enumerate((7.5, 8.2, 10.4, 13.0)):
        at(t, later, i * quarter, quarter)
    for k in range(NZ):
        at(3.8 + 2.64 * k, cot_forward, k)
        at(6.5 + 2.64 * k, grad, k)
        at(8.9 + 2.64 * k, pair_done, k)
    for s in range(1, 5):
        at(4.1 * s, w_z, s)
    for j in range(NZ):
        at(4.2 + 2.9 * j, w_y, j)
        at(7.2 + 2.9 * j, w_core, j)
    for d, times in enumerate(
        ((9.0, 11.7, 15.0, 18.9, 22.6, 26.5, 30.4), (9.0, 14.3, 15.1, 19.7, 22.7, 26.6, 30.5))
    ):
        for i, t in enumerate(times):
            at(t, chain, d, i)
    at(38.0, own_sum)
    at(43.5, grad_end)
    for j in range(NZ):
        at(17.0 + 2.6 * j, partial, j)
        at(22.0 + 2.9 * j, partial_on, j)
        at(27.0 + 2.9 * j, partial_end, j)
    for m in range(NX):
        at(35.8 + 1.8 * m, hidden, m)
        at(36.7 + 1.8 * m, pointwise, m)

    for _, _, run, args in sorted(tasks, key=lambda task: task[:2]):
        run(*args)
    for copy in sends:
        copy.wait_send()
    for copy in outs:
        copy.wait()


def on_device(lg, lu, eg, eu, cot, weight, running):
    tokens, block = lg.shape
    xrows, width = cot.shape
    dma, vmem = pltpu.SemaphoreType.DMA, pltpu.VMEM
    shape = jax.ShapeDtypeStruct
    pair = [dma((2, NZ))] * 2
    mixed, gate_grad, up_grad, summed = pl.pallas_call(
        kernel,
        out_shape=(
            shape((xrows, width), BF16),
            shape((tokens, block), BF16),
            shape((tokens, block), BF16),
            shape((ROWS, block), F32),
        ),
        in_specs=[pl.BlockSpec(memory_space=pl.ANY)] * 6,
        out_specs=[pl.BlockSpec(memory_space=pl.ANY)] * 4,
        scratch_shapes=[
            *[vmem((tokens, block), BF16)] * 5,
            vmem((tokens, width), BF16),
            vmem((NZ * NY, NC, ROWS, block), BF16),
            vmem((NZ, NY, NC, ROWS, block), BF16),
            vmem((NZ, NY, ROWS, block), BF16),
            vmem((2, 7, 2, ROWS, block), BF16),
            vmem((3, ROWS, block), BF16),
            vmem((NZ, NX, xrows, WIDE), BF16),
            vmem((2, NZ, xrows // 2, WIDE), BF16),
            vmem((2, NZ, xrows, WIDE), BF16),
            vmem((xrows, width), BF16),
            vmem((xrows, block), F32),
            vmem((ROWS, block), F32),
            dma((6,)),
            dma((17,)),
            *pair,
            *pair,
            *[dma((2, 4))] * 2,
            *pair,
            *pair,
            *[dma((NZ,))] * 2,
            *[dma((NZ,))] * 2,
            *[dma((2, 7))] * 2,
            *[dma((3,))] * 2,
            *pair,
            *pair,
        ],
        compiler_params=pltpu.CompilerParams(
            collective_id=0, has_side_effects=True, vmem_limit_bytes=60 * 1024 * 1024
        ),
        name="layer",
    )(lg, lu, eg, eu, cot, weight.T)
    return (mixed, gate_grad, up_grad, (running.T + summed).T)


def solution(mesh):
    tokens, hidden = P("fs", "tp"), P("tp", "fs")
    rows = P(("fs", "tp"), None)
    return jax.shard_map(
        on_device,
        mesh=mesh,
        in_specs=(tokens, tokens, tokens, tokens, rows, hidden, hidden),
        out_specs=(rows, tokens, tokens, hidden),
        check_vma=False,
    )
```

```python
import functools

import jax
import jax.numpy as jnp
from jax import lax
from jax.experimental import pallas as pl
from jax.experimental.pallas import tpu as pltpu
from jax.sharding import PartitionSpec as P

MESH = pl.DeviceIdType.MESH
F32, BF16 = jnp.float32, jnp.bfloat16
NX, NY, NZ, NC = 4, 4, 8, 2
ROWS = 32
WIDE = NY * NC * ROWS
TILE = 16


ORDER = (
    "B", "e0", "e1", "e2", "e3", "c", "L", "l0", "l1", "l2", "l3", "z1", "y0", "f0", "f1", "g0", "z2", "y1", "f2",
    "y2", "g1", "d0", "u0", "u1", "v0", "v1", "k0", "f3", "g2", "d1", "u2", "u3", "z3", "y3", "f4", "p0", "u4", "d2",
    "v2", "v3", "y4", "k1", "g3", "f5", "k2", "u5", "v4", "v5", "p1", "d3", "y5", "g4", "u6", "f6", "p2", "u7", "q0",
    "y6", "k3", "g5", "d4", "v6", "v7", "z4", "k4", "f7", "k5", "p3", "u8", "v8", "d5", "q1", "g6", "u9", "v9", "q2",
    "k6", "p4", "y7", "p5", "u10", "d6", "v10", "g7", "u11", "v11", "q3", "p6", "k7", "r0", "u12", "r1", "v12", "d7",
    "r2", "q4", "u13", "p7", "v13", "q5", "h0", "r3", "w0", "h1", "o2", "q6", "w1", "h2", "o0", "o1", "q7", "r4",
    "w2", "h3", "r5", "w3", "r6", "r7", "G",
)


def sigmoid(v):
    return 0.5 * jnp.tanh(0.5 * v) + 0.5


def kernel(
    lg_h, lu_h, eg_h, eu_h, cot_h, wt_h, running_h,
    mixed, eg, eu, gsum,
    lg, lu, eh, cot, wt, gbuf, precv, zrecv, yrecv, pbuf, pre, full, hc,
    load_sem, sent,
    cd_r, cf_r, wz_r, wy_r, wf_r, wd_r, gp_r, gz_r, gy_r, mp_r, mf_r,
):
    f, x = lax.axis_index("fs"), lax.axis_index("tp")
    c, y, z = lax.rem(f, NC), lax.rem(f // NC, NY), f // (NC * NY)
    xrows = cot_h.shape[0]
    half = xrows // 2
    hrow = ROWS // 2
    tokens = NX * xrows

    def dx(k):
        return lax.rem(x + (k + NX), NX)

    def dy(k):
        return lax.rem(y + (k + NY), NY)

    def dz(k):
        return lax.rem(z + (k + NZ), NZ)

    def at_x(k):
        return (f, dx(k))

    def at_y(k):
        return ((z * NY + dy(k)) * NC + c, x)

    def at_z(k):
        return ((dz(k) * NY + y) * NC + c, x)

    partner = ((z * NY + y) * NC + (1 - c), x)

    def send(src, dst, kind, rsem, to):
        pltpu.make_async_remote_copy(
            src_ref=src, dst_ref=dst, send_sem=sent.at[kind], recv_sem=rsem, device_id=to, device_id_type=MESH
        ).start()

    def arrived(dst, rsem):
        pltpu.make_async_remote_copy(
            src_ref=dst, dst_ref=dst, send_sem=sent.at[0], recv_sem=rsem, device_id=partner, device_id_type=MESH
        ).wait_recv()

    def all_sent(kind, like):
        pltpu.make_async_remote_copy(
            src_ref=like, dst_ref=like, send_sem=sent.at[kind], recv_sem=cd_r.at[0, 0], device_id=partner, device_id_type=MESH
        ).wait_send()

    loads = [
        pltpu.make_async_copy(src, dst, load_sem.at[i])
        for i, (src, dst) in enumerate(
            [
                (eg_h, eg),
                (eu_h, eu),
                (cot_h, cot.at[pl.ds(pl.multiple_of(x * xrows, TILE), xrows)]),
                (wt_h, wt.at[z * NY + y, c]),
                (lg_h, lg),
                (lu_h, lu),
                (running_h, gsum),
            ]
        )
    ]
    for copy in loads:
        copy.start()

    barrier = pltpu.get_barrier_semaphore()
    peers = [at_x(1), at_x(-1), at_y(1), at_y(-1), at_y(2), at_z(1), at_z(-1), partner]
    for peer in peers:
        pl.semaphore_signal(barrier, inc=1, device_id=peer, device_id_type=MESH)
    pl.semaphore_wait(barrier, len(peers))

    SIDES = ((0, 1), (1, -1))
    ZSTEPS = (4, 3, -3, 2, -2, 1, -1, 0)
    WSTEPS = (0, -1, 1, -2, 2, -3, 3, 4)

    def columns(step):
        return pl.ds(pl.multiple_of(dz(step) * WIDE, WIDE), WIDE)

    def cot_rows(step, start=0, size=xrows):
        return pl.ds(pl.multiple_of(dx(step) * xrows + start, TILE), size)

    def cot_direct(k):
        cols = columns(ZSTEPS[k])
        for d, s in SIDES:
            send(cot_h.at[:, cols], cot.at[cot_rows(0), cols], 0, cd_r.at[d, k], at_x(s))

    def cot_forward(k):
        cols = columns(ZSTEPS[k])
        for d, s in SIDES:
            block = cot.at[cot_rows(-s), cols]
            arrived(block, cd_r.at[d, k])
            part = cot.at[cot_rows(-s, d * half, half), cols]
            send(part, part, 1, cf_r.at[d, k], at_x(s))
        if k + 2 < NZ:
            cot_direct(k + 2)

    def cot_done(k):
        cols = columns(ZSTEPS[k])
        for d, s in SIDES:
            part = cot.at[cot_rows(2, d * half, half), cols]
            arrived(part, cf_r.at[d, k])

    def w_block(zs, ys):
        return wt.at[dz(zs) * NY + dy(ys), c]

    def w_along_z(s):
        for d, step in SIDES:
            block = w_block(-step * (s - 1), 0)
            if s == 4:
                block = block.at[pl.ds(d * hrow, hrow)]
            send(block, block, 2, wz_r.at[d, s - 1], at_z(step))

    def w_along_y(j):
        block = w_block(WSTEPS[j], 0)
        for d, step in SIDES:
            send(block, block, 3, wy_r.at[d, j], at_y(step))

    def w_z(s):
        for d, step in SIDES:
            block = w_block(-step * s, 0)
            if s == 4:
                block = block.at[pl.ds(d * hrow, hrow)]
            arrived(block, wz_r.at[d, s - 1])
        if s < 4:
            w_along_z(s + 1)
            w_along_y(2 * s - 1)
            w_along_y(2 * s)
        else:
            w_along_y(7)

    def w_y(j):
        for d, step in SIDES:
            block = w_block(WSTEPS[j], -step)
            arrived(block, wy_r.at[d, j])
            part = block.at[pl.ds(d * hrow, hrow)]
            send(part, part, 4, wf_r.at[d, j], at_y(step))

    def w_core(j):
        for d, step in SIDES:
            part = w_block(WSTEPS[j], 2).at[pl.ds(d * hrow, hrow)]
            arrived(part, wf_r.at[d, j])
        rows = wt.at[pl.ds(dz(WSTEPS[j]) * NY, NY), c]
        send(rows, rows, 5, wd_r.at[j], partner)

    def w_done(j):
        rows = wt.at[pl.ds(dz(WSTEPS[j]) * NY, NY), 1 - c]
        arrived(rows, wd_r.at[j])

    def over_rows(first, size, body):
        def step(i, carry):
            body(pl.ds(pl.multiple_of(first + i * TILE, TILE), TILE))
            return carry

        lax.fori_loop(0, size // TILE, step, 0)

    def early(first, size):
        def body(rows):
            gate = eg[rows, :].astype(F32)
            eh[rows, :] = (gate * sigmoid(gate) * eu[rows, :].astype(F32)).astype(BF16)

        over_rows(first, size, body)

    def later(first, size):
        def body(rows):
            gate = lg[rows, :].astype(F32)
            lg[rows, :] = (gate * sigmoid(gate) * lu[rows, :].astype(F32)).astype(BF16)

        over_rows(first, size, body)

    def grad(k):
        cot_done(k)
        part = lax.dot_general(
            cot[:, columns(ZSTEPS[k])], eh[...], (((0,), (0,)), ((), ())), preferred_element_type=F32
        )
        gbuf[k] = part.astype(BF16).reshape(NY, NC, ROWS, part.shape[1])
        send(gbuf.at[k, :, 1 - c], precv.at[k], 6, gp_r.at[k], partner)

    def pair_done(k):
        arrived(precv.at[k], gp_r.at[k])

    def add_up(k, r, more):
        total = gbuf[k, dy(r), c].astype(F32) + precv[k, dy(r)].astype(F32)
        for d, i in more:
            total += zrecv[d, i].astype(F32)
        return total

    CHAIN = (
        ((0, -1), (0, 0), *((k, r) for k in (1, 3, 5) for r in (2, 1, -1, 0))),
        ((0, 2), (0, 1), *((k, r) for k in (2, 4, 6) for r in (-1, 2, 1, 0))),
    )

    def chain_before(d, k, r):
        nearer = ((1, 3, 5, 7), (2, 4, 6, 7))[d]
        before = (((0,) + nearer)[nearer.index(k)], r) if k in nearer else None
        if before not in CHAIN[d]:
            return []
        i = CHAIN[d].index(before)
        arrived(zrecv.at[d, i], gz_r.at[d, i])
        return [(d, i)]

    def chain(d, i):
        k, r = CHAIN[d][i]
        gbuf[k, dy(r), c] = add_up(k, r, chain_before(d, k, r)).astype(BF16)
        send(gbuf.at[k, dy(r), c], zrecv.at[d, i], 7, gz_r.at[d, i], at_z(SIDES[d][1]))

    def own_sum(i):
        r = (1, -1, 2)[i]
        gbuf[7, dy(r), c] = add_up(7, r, chain_before(0, 7, r) + chain_before(1, 7, r)).astype(BF16)
        send(gbuf.at[7, dy(r), c], yrecv.at[i], 8, gy_r.at[i], at_y(r))

    def grad_end():
        total = add_up(7, 0, chain_before(0, 7, 0) + chain_before(1, 7, 0))
        for i in range(3):
            arrived(yrecv.at[i], gy_r.at[i])
            total += yrecv[i].astype(F32)
        gsum[...] += total

    def partial(j):
        w_done(j)
        rows = wt[pl.ds(dz(WSTEPS[j]) * NY, NY)].reshape(WIDE, wt.shape[3])
        part = lax.dot_general(lg[...], rows, (((1,), (1,)), ((), ())), preferred_element_type=F32)
        pbuf[j] = part.astype(BF16).reshape(NX, xrows, WIDE)
        for d, s in SIDES:
            send(pbuf.at[j, dx(2), pl.ds(d * half, half)], pre.at[d, j], 9, mp_r.at[d, j], at_x(s))

    def partial_on(j):
        for d, s in SIDES:
            arrived(pre.at[d, j], mp_r.at[d, j])
            rows = pl.ds(d * half, half)
            pbuf[j, dx(s), rows] = (pbuf[j, dx(s), rows].astype(F32) + pre[d, j].astype(F32)).astype(BF16)
            send(pbuf.at[j, dx(s)], full.at[d, j], 10, mf_r.at[d, j], at_x(s))

    def partial_end(j):
        total = pbuf[j, x].astype(F32)
        for d, s in SIDES:
            arrived(full.at[d, j], mf_r.at[d, j])
            total += full[d, j].astype(F32)
        cols = columns(WSTEPS[j])
        mixed[:, cols] = total.astype(BF16)

    def hidden(m):
        rows = pl.ds(m * xrows, xrows)
        hc[...] = jnp.dot(
            cot[rows, :], wt[...].reshape(NZ * WIDE, wt.shape[3]), preferred_element_type=F32
        )

    def pointwise(m):
        def body(rows):
            sub = pl.ds(rows.start - m * xrows, TILE)
            gate, up, cotan = eg[rows, :].astype(F32), eu[rows, :].astype(F32), hc[sub, :]
            s = sigmoid(gate)
            scaled = cotan * s
            eg[rows, :] = (scaled * up * (1.0 + gate * (1.0 - s))).astype(BF16)
            eu[rows, :] = (scaled * gate).astype(BF16)

        over_rows(m * xrows, xrows, body)

    def begin():
        cot_direct(0)
        loads[3].wait()
        w_along_z(1)
        w_along_y(0)
        cot_direct(1)
        loads[0].wait()
        loads[1].wait()

    def later_loads():
        for copy in loads[4:]:
            copy.wait()

    quarter = tokens // 4
    tasks = {
        "B": begin,
        "e": lambda i: early(i * quarter, quarter),
        "c": loads[2].wait,
        "L": later_loads,
        "l": lambda i: later(i * quarter, quarter),
        "f": cot_forward,
        "g": grad,
        "d": pair_done,
        "z": w_z,
        "y": w_y,
        "k": w_core,
        "u": lambda i: chain(0, i),
        "v": lambda i: chain(1, i),
        "o": own_sum,
        "G": grad_end,
        "p": partial,
        "q": partial_on,
        "r": partial_end,
        "h": hidden,
        "w": pointwise,
    }
    for task in ORDER:
        tasks[task[0]](*(int(i) for i in task[1:].split("_") if i))
    for kind, like in enumerate(
        (full, pre, wt.at[pl.ds(0, 7), 0], wt.at[pl.ds(0, 16), 0], wt.at[pl.ds(0, 8), 0], precv, precv,
         wt.at[pl.ds(0, 28), 0], yrecv, pre, full)
    ):
        all_sent(kind, like)


def on_device(lg, lu, eg, eu, cot, weight, running):
    tokens, block = lg.shape
    xrows, width = cot.shape
    dma, vmem = pltpu.SemaphoreType.DMA, pltpu.VMEM
    mixed, gate_grad, up_grad, total = pl.pallas_call(
        kernel,
        out_shape=(
            vmem((xrows, width), BF16),
            vmem((tokens, block), BF16),
            vmem((tokens, block), BF16),
            vmem((ROWS, block), F32),
        ),
        in_specs=[pl.BlockSpec(memory_space=pl.ANY)] * 7,
        out_specs=[pl.BlockSpec(memory_space=vmem)] * 4,
        scratch_shapes=[
            *[vmem((tokens, block), BF16)] * 3,
            vmem((tokens, width), BF16),
            vmem((NZ * NY, NC, ROWS, block), BF16),
            vmem((NZ, NY, NC, ROWS, block), BF16),
            vmem((NZ, NY, ROWS, block), BF16),
            vmem((2, 14, ROWS, block), BF16),
            vmem((3, ROWS, block), BF16),
            vmem((NZ, NX, xrows, WIDE), BF16),
            vmem((2, NZ, xrows // 2, WIDE), BF16),
            vmem((2, NZ, xrows, WIDE), BF16),
            vmem((xrows, block), F32),
            dma((7,)),
            dma((11,)),
            dma((2, NZ)),
            dma((2, NZ)),
            dma((2, 4)),
            dma((2, NZ)),
            dma((2, NZ)),
            dma((NZ,)),
            dma((NZ,)),
            dma((2, 14)),
            dma((3,)),
            dma((2, NZ)),
            dma((2, NZ)),
        ],
        compiler_params=pltpu.CompilerParams(
            collective_id=0, has_side_effects=True, vmem_limit_bytes=52 * 1024 * 1024
        ),
        name="layer",
    )(lg, lu, eg, eu, cot, weight.T, running.T)
    return (mixed, gate_grad, up_grad, total.T)


def solution(mesh):
    tokens, hidden = P("fs", "tp"), P("tp", "fs")
    rows = P(("fs", "tp"), None)
    return jax.shard_map(
        on_device,
        mesh=mesh,
        in_specs=(tokens, tokens, tokens, tokens, rows, hidden, hidden),
        out_specs=(rows, tokens, tokens, hidden),
        check_vma=False,
    )
```

```python
import functools

import jax
import jax.numpy as jnp
from jax import lax
from jax.experimental import pallas as pl
from jax.experimental.pallas import tpu as pltpu
from jax.sharding import PartitionSpec as P

MESH = pl.DeviceIdType.MESH
F32, BF16 = jnp.float32, jnp.bfloat16
NX, NY, NZ, NC = 4, 4, 8, 2
ROWS = 32
WIDE = NY * NC * ROWS
TILE = 16
AHEAD = ((2,), (3,), (4, 5), (6,), (7,), (), (), ())
CUT = 1024
KCUT = 768
PARTS = 2


ORDER = (
    "B", "e0", "e1", "e2", "e3", "c", "L", "l0", "l1", "l2", "z1_0", "l3", "z1_1", "y0", "f0", "f1", "z2_0", "g0",
    "z2_1", "y1", "f2", "z3_0", "g1", "d0", "u0", "u1", "v0", "v1", "y2", "k0", "z3_1", "f3", "z4_0", "g2", "d1",
    "u2", "u3", "y3", "f4", "p0", "u4", "y4", "d2", "v2", "v3", "k1", "f5", "k2", "u5", "v4", "v5", "g3", "z4_1",
    "p1", "f6", "y5", "p2", "g4", "d3", "u6", "y6", "u7", "f7", "k3", "q0", "d4", "v6", "u8", "v7", "k4", "g5", "v8",
    "q1", "p3", "u9", "y7", "p4", "v9", "k5", "g6", "d5", "u10", "q2", "k6", "g7", "p5", "u11", "k7", "r0", "d6",
    "v10", "p6", "r1", "d7", "u12", "p7", "v11", "v12", "q3", "h0_0", "u13", "q4", "h0_1", "v13", "w0", "r2", "h1_0",
    "q5", "h1_1", "o0", "q6", "w1", "h2_0", "q7", "h2_1", "o1", "w2", "r3", "h3_0", "o2", "h3_1", "w3", "r4", "r5",
    "r6", "G", "r7",
)


def sigmoid(v):
    return 0.5 * jnp.tanh(0.5 * v) + 0.5


def kernel(
    lg_h, lu_h, eg_h, eu_h, cot_h, wt_h, running_h,
    mixed, eg, eu, gsum,
    lg, lu, eh, cot, wt, gbuf, precv, zrecv, yrecv, pbuf, pre, full, hc,
    load_sem, sent,
    cd_r, cf_r, wz_r, wy_r, wf_r, wd_r, gp_r, gz_r, gy_r, mp_r, mf_r,
):
    f, x = lax.axis_index("fs"), lax.axis_index("tp")
    c, y, z = lax.rem(f, NC), lax.rem(f // NC, NY), f // (NC * NY)
    xrows = cot_h.shape[0]
    half = xrows // 2
    hrow = ROWS // 2
    tokens = NX * xrows

    def dx(k):
        return lax.rem(x + (k + NX), NX)

    def dy(k):
        return lax.rem(y + (k + NY), NY)

    def dz(k):
        return lax.rem(z + (k + NZ), NZ)

    def at_x(k):
        return (f, dx(k))

    def at_y(k):
        return ((z * NY + dy(k)) * NC + c, x)

    def at_z(k):
        return ((dz(k) * NY + y) * NC + c, x)

    partner = ((z * NY + y) * NC + (1 - c), x)

    def send(src, dst, kind, rsem, to):
        pltpu.make_async_remote_copy(
            src_ref=src, dst_ref=dst, send_sem=sent.at[kind], recv_sem=rsem, device_id=to, device_id_type=MESH
        ).start()

    def arrived(dst, rsem):
        pltpu.make_async_remote_copy(
            src_ref=dst, dst_ref=dst, send_sem=sent.at[0], recv_sem=rsem, device_id=partner, device_id_type=MESH
        ).wait_recv()

    def all_sent(kind, like):
        pltpu.make_async_remote_copy(
            src_ref=like, dst_ref=like, send_sem=sent.at[kind], recv_sem=cd_r.at[0], device_id=partner, device_id_type=MESH
        ).wait_send()

    barrier = pltpu.get_barrier_semaphore()
    peers = [at_x(1), at_x(-1), at_y(1), at_y(-1), at_y(2), at_z(1), at_z(-1), partner]
    for peer in peers:
        pl.semaphore_signal(barrier, inc=1, device_id=peer, device_id_type=MESH)

    loads = [
        pltpu.make_async_copy(src, dst, load_sem.at[i])
        for i, (src, dst) in enumerate(
            [
                (eg_h, eg),
                (eu_h, eu),
                (cot_h, cot.at[pl.ds(pl.multiple_of(x * xrows, TILE), xrows)]),
                (wt_h, wt.at[z * NY + y, c]),
                (lg_h, lg),
                (lu_h, lu),
                (running_h, gsum),
            ]
        )
    ]
    for copy in loads:
        copy.start()

    pl.semaphore_wait(barrier, len(peers))

    SIDES = ((0, 1), (1, -1))
    ZSTEPS = (4, 3, -3, 2, -2, 1, -1, 0)
    WSTEPS = (0, -1, 1, -2, 2, -3, 3, 4)

    def columns(step):
        return pl.ds(pl.multiple_of(dz(step) * WIDE, WIDE), WIDE)

    def cot_rows(step, start=0, size=xrows):
        return pl.ds(pl.multiple_of(dx(step) * xrows + start, TILE), size)

    def cot_direct(k):
        cols = columns(ZSTEPS[k])
        for d, s in SIDES:
            send(cot_h.at[:, cols], cot.at[cot_rows(0), cols], 0, cd_r.at[k], at_x(s))

    def cot_forward(k):
        cols = columns(ZSTEPS[k])
        arrived(full.at[:, 0], cd_r.at[k])
        for d, s in SIDES:
            part = cot.at[cot_rows(-s, d * half, half), cols]
            send(part, part, 1, cf_r.at[k], at_x(s))
        for ahead in AHEAD[k]:
            cot_direct(ahead)

    def cot_done(k):
        arrived(pre.at[:, 0], cf_r.at[k])

    def w_block(zs, ys):
        return wt.at[dz(zs) * NY + dy(ys), c]

    def w_along_z(s, h):
        for d, step in SIDES:
            if s < 4 or d == h:
                part = w_block(-step * (s - 1), 0).at[pl.ds(h * hrow, hrow)]
                send(part, part, 2, wz_r.at[s - 1, h], at_z(step))

    def w_along_y(j):
        block = w_block(WSTEPS[j], 0)
        for d, step in SIDES:
            send(block, block, 3, wy_r.at[j], at_y(step))

    def w_z(s, h):
        arrived(wt.at[0, 0] if s < 4 else wt.at[0, 0, pl.ds(0, hrow)], wz_r.at[s - 1, h])
        if s < 4:
            w_along_z(s + 1, h)
        if h == 1:
            for j in (2 * s - 1, 2 * s) if s < 4 else (7,):
                w_along_y(j)

    def w_y(j):
        arrived(wt.at[0], wy_r.at[j])
        for d, step in SIDES:
            part = w_block(WSTEPS[j], -step).at[pl.ds(d * hrow, hrow)]
            send(part, part, 4, wf_r.at[j], at_y(step))

    def w_core(j):
        arrived(wt.at[0, 0], wf_r.at[j])
        rows = wt.at[pl.ds(dz(WSTEPS[j]) * NY, NY), c]
        send(rows, rows, 5, wd_r.at[j], partner)

    def w_done(j):
        rows = wt.at[pl.ds(dz(WSTEPS[j]) * NY, NY), 1 - c]
        arrived(rows, wd_r.at[j])

    def alone(run):
        pl.when(f >= 0)(run)

    def over_rows(first, size, body):
        def step(i, carry):
            body(pl.ds(pl.multiple_of(first + i * TILE, TILE), TILE))
            return carry

        lax.fori_loop(0, size // TILE, step, 0)

    def early(first, size):
        def body(rows):
            gate = eg[rows, :].astype(F32)
            eh[rows, :] = (gate * sigmoid(gate) * eu[rows, :].astype(F32)).astype(BF16)

        over_rows(first, size, body)

    def later(first, size):
        def body(rows):
            gate = lg[rows, :].astype(F32)
            lg[rows, :] = (gate * sigmoid(gate) * lu[rows, :].astype(F32)).astype(BF16)

        over_rows(first, size, body)

    def grad(k):
        cot_done(k)

        @alone
        def _():
            part = lax.dot_general(
                cot[:, columns(ZSTEPS[k])], eh[...], (((0,), (0,)), ((), ())), preferred_element_type=F32
            )
            gbuf[k] = part.astype(BF16).reshape(NY, NC, ROWS, part.shape[1])

        send(gbuf.at[k, :, 1 - c], precv.at[k], 6, gp_r.at[k], partner)

    def pair_done(k):
        arrived(precv.at[k], gp_r.at[k])

    def add_up(k, r, more):
        total = gbuf[k, dy(r), c].astype(F32) + precv[k, dy(r)].astype(F32)
        for d, i in more:
            total += zrecv[d, i].astype(F32)
        return total

    CHAIN = (
        ((0, -1), (0, 0), *((k, r) for k in (1, 3, 5) for r in (2, 1, -1, 0))),
        ((0, 2), (0, 1), (2, -1), (2, 2), (2, 1), (2, 0), (4, 2), (4, -1), (4, 1), (4, 0), (6, 2), (6, 1), (6, -1), (6, 0)),
    )

    def chain_before(d, k, r):
        nearer = ((1, 3, 5, 7), (2, 4, 6, 7))[d]
        before = (((0,) + nearer)[nearer.index(k)], r) if k in nearer else None
        if before not in CHAIN[d]:
            return []
        i = CHAIN[d].index(before)
        arrived(zrecv.at[d, i], gz_r.at[d, i])
        return [(d, i)]

    def chain(d, i):
        k, r = CHAIN[d][i]
        gbuf[k, dy(r), c] = add_up(k, r, chain_before(d, k, r)).astype(BF16)
        send(gbuf.at[k, dy(r), c], zrecv.at[d, i], 7, gz_r.at[d, i], at_z(SIDES[d][1]))

    def own_sum(i):
        r = (2, 1, -1)[i]
        gbuf[7, dy(r), c] = add_up(7, r, chain_before(0, 7, r) + chain_before(1, 7, r)).astype(BF16)
        send(gbuf.at[7, dy(r), c], yrecv.at[i], 8, gy_r.at[0], at_y(r))

    def grad_end():
        total = add_up(7, 0, chain_before(0, 7, 0) + chain_before(1, 7, 0))
        arrived(yrecv, gy_r.at[0])
        for i in range(3):
            total += yrecv[i].astype(F32)
        gsum[...] += total

    def partial(j):
        w_done(j)

        @alone
        def _():
            at = pl.ds(dz(WSTEPS[j]) * NY, NY)

            def product(cols, sign):
                rows = sign * wt[at, :, :, cols].reshape(WIDE, -1)
                return lax.dot_general(lg[:, cols], rows, (((1,), (1,)), ((), ())), preferred_element_type=F32)

            part = product(slice(0, KCUT), 1) - product(slice(KCUT, None), -1)
            pbuf[j] = part.astype(BF16).reshape(NX, xrows, WIDE)

        for d, s in SIDES:
            send(pbuf.at[j, dx(2), pl.ds(d * half, half)], pre.at[d, j], 9, mp_r.at[j], at_x(s))

    def partial_on(j):
        arrived(pre.at[:, 0], mp_r.at[j])
        for d, s in SIDES:
            rows = pl.ds(d * half, half)
            pbuf[j, dx(s), rows] = (pbuf[j, dx(s), rows].astype(F32) + pre[d, j].astype(F32)).astype(BF16)
            send(pbuf.at[j, dx(s)], full.at[d, j], 10, mf_r.at[j], at_x(s))

    def partial_end(j):
        arrived(full.at[:, 0], mf_r.at[j])
        total = pbuf[j, x].astype(F32) + full[0, j].astype(F32) + full[1, j].astype(F32)
        mixed[:, columns(WSTEPS[j])] = total.astype(BF16)

    def hidden(m, i):
        rows = pl.ds(m * xrows, xrows)
        cols = (slice(0, CUT), slice(CUT, None))[i]

        @alone
        def _():
            hc[:, cols] = jnp.dot(
                cot[rows, :], wt[:, :, :, cols].reshape(NZ * WIDE, -1), preferred_element_type=F32
            )


    def pointwise(m):
        def body(rows):
            sub = pl.ds(rows.start - m * xrows, TILE)
            gate, up, cotan = eg[rows, :].astype(F32), eu[rows, :].astype(F32), hc[sub, :]
            s = sigmoid(gate)
            scaled = cotan * s
            eg[rows, :] = (scaled * up * (1.0 + gate * (1.0 - s))).astype(BF16)
            eu[rows, :] = (scaled * gate).astype(BF16)

        over_rows(m * xrows, xrows, body)

    def begin():
        cot_direct(0)
        loads[3].wait()
        w_along_z(1, 0)
        w_along_z(1, 1)
        w_along_y(0)
        cot_direct(1)
        loads[0].wait()
        loads[1].wait()

    def later_loads():
        for copy in loads[4:]:
            copy.wait()

    quarter = tokens // 4
    tasks = {
        "B": begin,
        "e": lambda i: early(i * quarter, quarter),
        "c": loads[2].wait,
        "L": later_loads,
        "l": lambda i: later(i * quarter, quarter),
        "f": cot_forward,
        "g": grad,
        "d": pair_done,
        "z": w_z,
        "y": w_y,
        "k": w_core,
        "u": lambda i: chain(0, i),
        "v": lambda i: chain(1, i),
        "o": own_sum,
        "G": grad_end,
        "p": partial,
        "q": partial_on,
        "r": partial_end,
        "h": hidden,
        "w": pointwise,
    }
    for task in ORDER:
        tasks[task[0]](*(int(i) for i in task[1:].split("_") if i))
    for kind, like in enumerate(
        (full, pre, wt.at[pl.ds(0, 7), 0], wt.at[pl.ds(0, 16), 0], wt.at[pl.ds(0, 8), 0], precv, precv,
         wt.at[pl.ds(0, 28), 0], yrecv, pre, full)
    ):
        all_sent(kind, like)


def put_kernel(*refs):
    *refs, sem = refs
    half = len(refs) // 2
    copies = []
    for src, dst in zip(refs[:half], refs[half:]):
        rows = src.shape[0] // PARTS
        for i in range(PARTS):
            at = pl.ds(i * rows, rows)
            copies.append(pltpu.make_async_copy(src.at[at], dst.at[at], sem.at[len(copies)]))
    for copy in copies:
        copy.start()
    for copy in copies:
        copy.wait()


def on_device(lg, lu, eg, eu, cot, weight, running):
    tokens, block = lg.shape
    xrows, width = cot.shape
    dma, vmem = pltpu.SemaphoreType.DMA, pltpu.VMEM
    mixed, gate_grad, up_grad, total = pl.pallas_call(
        kernel,
        out_shape=(
            vmem((xrows, width), BF16),
            vmem((tokens, block), BF16),
            vmem((tokens, block), BF16),
            vmem((ROWS, block), F32),
        ),
        in_specs=[pl.BlockSpec(memory_space=pl.ANY)] * 7,
        out_specs=[pl.BlockSpec(memory_space=vmem)] * 4,
        scratch_shapes=[
            *[vmem((tokens, block), BF16)] * 3,
            vmem((tokens, width), BF16),
            vmem((NZ * NY, NC, ROWS, block), BF16),
            vmem((NZ, NY, NC, ROWS, block), BF16),
            vmem((NZ, NY, ROWS, block), BF16),
            vmem((2, 14, ROWS, block), BF16),
            vmem((3, ROWS, block), BF16),
            vmem((NZ, NX, xrows, WIDE), BF16),
            vmem((2, NZ, xrows // 2, WIDE), BF16),
            vmem((2, NZ, xrows, WIDE), BF16),
            vmem((xrows, block), F32),
            dma((7,)),
            dma((11,)),
            dma((NZ,)),
            dma((NZ,)),
            dma((4, 2)),
            dma((NZ,)),
            dma((NZ,)),
            dma((NZ,)),
            dma((NZ,)),
            dma((2, 14)),
            dma((1,)),
            dma((NZ,)),
            dma((NZ,)),
        ],
        compiler_params=pltpu.CompilerParams(
            collective_id=0, has_side_effects=True, vmem_limit_bytes=52 * 1024 * 1024
        ),
        name="layer",
    )(lg, lu, eg, eu, cot, weight.T, running.T)
    results = (gate_grad, up_grad, mixed, total)
    gate_grad, up_grad, mixed, total = pl.pallas_call(
        put_kernel,
        out_shape=[jax.ShapeDtypeStruct(v.shape, v.dtype) for v in results],
        in_specs=[pl.BlockSpec(memory_space=vmem)] * 4,
        out_specs=[pl.BlockSpec(memory_space=pl.ANY)] * 4,
        scratch_shapes=[dma((4 * PARTS,))],
        compiler_params=pltpu.CompilerParams(vmem_limit_bytes=1 << 20),
        name="put",
    )(*results)
    return (mixed, gate_grad, up_grad, total.T)


def solution(mesh):
    tokens, hidden = P("fs", "tp"), P("tp", "fs")
    rows = P(("fs", "tp"), None)
    return jax.shard_map(
        on_device,
        mesh=mesh,
        in_specs=(tokens, tokens, tokens, tokens, rows, hidden, hidden),
        out_specs=(rows, tokens, tokens, hidden),
        check_vma=False,
    )
```

```python
import functools

import jax
import jax.numpy as jnp
from jax import lax
from jax.experimental import pallas as pl
from jax.experimental.pallas import tpu as pltpu
from jax.sharding import PartitionSpec as P

MESH = pl.DeviceIdType.MESH
F32, BF16 = jnp.float32, jnp.bfloat16
NX, NY, NZ, NC = 4, 4, 8, 2
ROWS = 32
WIDE = NY * NC * ROWS
TILE = 16
AHEAD = ((), (3,), (4,), (5,), (6,), (7,), (), ())
CUT = 1024
KCUT = 768
PARTS = (1, 1, 1, 1)


ORDER = (
    "B", "e0", "e1", "e2", "e3", "c", "L", "l0", "l1", "l2", "l3", "z1_0", "z1_1", "y0", "f0", "f1", "z2_0", "f2",
    "z2_1", "y1", "g0", "g1", "z3_0", "y2", "z3_1", "f3", "k0", "d0", "u0", "u1", "v0", "v1", "g2", "d1", "u2", "u3",
    "y3", "z4_0", "f4", "p0", "z4_1", "g3", "d2", "v2", "y4", "u4", "k1", "v3", "f5", "k2", "g4", "d3", "u5", "v4",
    "v5", "f6", "p1", "u6", "y5", "q0", "d4", "g5", "u7", "y6", "k3", "v6", "v7", "f7", "p2", "g6", "d5", "u8", "v8",
    "q1", "y7", "p3", "k4", "u9", "k5", "v9", "r0", "d6", "k6", "g7", "u10", "v10", "q2", "k7", "p4", "p5", "u11",
    "p6", "d7", "r1", "q3", "p7", "u12", "h0_0", "v11", "v12", "r2", "h0_1", "w0", "u13", "q4", "v13", "h1_0", "q5",
    "h1_1", "q6", "w1", "o0", "h2_0", "r3", "h2_1", "w2", "o1", "q7", "h3_0", "h3_1", "w3", "o2", "r4", "r5", "r6",
    "G", "r7",
)


def sigmoid(v):
    return 0.5 * jnp.tanh(0.5 * v) + 0.5


def kernel(
    lg_h, lu_h, eg_h, eu_h, cot_h, wt_h, running_h,
    mixed, eg, eu, gsum,
    lg, lu, eh, cot, wt, gbuf, precv, zrecv, yrecv, pbuf, pre, full, hc,
    load_sem, sent,
    cd_r, cf_r, wz_r, wy_r, wf_r, wd_r, gp_r, gz_r, gy_r, mp_r, mf_r,
):
    f, x = lax.axis_index("fs"), lax.axis_index("tp")
    c, y, z = lax.rem(f, NC), lax.rem(f // NC, NY), f // (NC * NY)
    xrows = cot_h.shape[0]
    half = xrows // 2
    hrow = ROWS // 2
    tokens = NX * xrows

    def dx(k):
        return lax.rem(x + (k + NX), NX)

    def dy(k):
        return lax.rem(y + (k + NY), NY)

    def dz(k):
        return lax.rem(z + (k + NZ), NZ)

    def at_x(k):
        return (f, dx(k))

    def at_y(k):
        return ((z * NY + dy(k)) * NC + c, x)

    def at_z(k):
        return ((dz(k) * NY + y) * NC + c, x)

    partner = ((z * NY + y) * NC + (1 - c), x)

    def send(src, dst, kind, rsem, to):
        pltpu.make_async_remote_copy(
            src_ref=src, dst_ref=dst, send_sem=sent.at[kind], recv_sem=rsem, device_id=to, device_id_type=MESH
        ).start()

    def arrived(dst, rsem):
        pltpu.make_async_remote_copy(
            src_ref=dst, dst_ref=dst, send_sem=sent.at[0], recv_sem=rsem, device_id=partner, device_id_type=MESH
        ).wait_recv()

    def all_sent(kind, like):
        pltpu.make_async_remote_copy(
            src_ref=like, dst_ref=like, send_sem=sent.at[kind], recv_sem=cd_r.at[0], device_id=partner, device_id_type=MESH
        ).wait_send()

    barrier = pltpu.get_barrier_semaphore()
    peers = [at_x(1), at_x(-1), at_y(1), at_y(-1), at_y(2), at_z(1), at_z(-1), partner]
    for peer in peers:
        pl.semaphore_signal(barrier, inc=1, device_id=peer, device_id_type=MESH)

    loads = [
        pltpu.make_async_copy(src, dst, load_sem.at[i])
        for i, (src, dst) in enumerate(
            [
                (eg_h, eg),
                (eu_h, eu),
                (cot_h, cot.at[pl.ds(pl.multiple_of(x * xrows, TILE), xrows)]),
                (wt_h, wt.at[z * NY + y, c]),
                (lg_h, lg),
                (lu_h, lu),
                (running_h, gsum),
            ]
        )
    ]
    for copy in loads:
        copy.start()

    pl.semaphore_wait(barrier, len(peers))

    SIDES = ((0, 1), (1, -1))
    ZSTEPS = (4, 3, -3, 2, -2, 1, -1, 0)
    WSTEPS = (0, -1, 1, -2, 2, -3, 3, 4)

    def columns(step):
        return pl.ds(pl.multiple_of(dz(step) * WIDE, WIDE), WIDE)

    def cot_rows(step, start=0, size=xrows):
        return pl.ds(pl.multiple_of(dx(step) * xrows + start, TILE), size)

    def cot_direct(k):
        cols = columns(ZSTEPS[k])
        for d, s in SIDES:
            send(cot_h.at[:, cols], cot.at[cot_rows(0), cols], 0, cd_r.at[k], at_x(s))

    def cot_forward(k):
        cols = columns(ZSTEPS[k])
        arrived(full.at[:, 0], cd_r.at[k])
        for d, s in SIDES:
            part = cot.at[cot_rows(-s, d * half, half), cols]
            send(part, part, 1, cf_r.at[k], at_x(s))
        for ahead in AHEAD[k]:
            cot_direct(ahead)

    def cot_done(k):
        arrived(pre.at[:, 0], cf_r.at[k])

    def w_block(zs, ys):
        return wt.at[dz(zs) * NY + dy(ys), c]

    def w_along_z(s, h):
        for d, step in SIDES:
            if s < 4 or d == h:
                part = w_block(-step * (s - 1), 0).at[pl.ds(h * hrow, hrow)]
                send(part, part, 2, wz_r.at[s - 1, h], at_z(step))

    def w_along_y(j):
        block = w_block(WSTEPS[j], 0)
        for d, step in SIDES:
            send(block, block, 3, wy_r.at[j], at_y(step))

    def w_z(s, h):
        arrived(wt.at[0, 0] if s < 4 else wt.at[0, 0, pl.ds(0, hrow)], wz_r.at[s - 1, h])
        if s < 4:
            w_along_z(s + 1, h)
        if h == 1:
            for j in (2 * s - 1, 2 * s) if s < 4 else (7,):
                w_along_y(j)

    def w_y(j):
        arrived(wt.at[0], wy_r.at[j])
        for d, step in SIDES:
            part = w_block(WSTEPS[j], -step).at[pl.ds(d * hrow, hrow)]
            send(part, part, 4, wf_r.at[j], at_y(step))

    def w_core(j):
        arrived(wt.at[0, 0], wf_r.at[j])
        rows = wt.at[pl.ds(dz(WSTEPS[j]) * NY, NY), c]
        send(rows, rows, 5, wd_r.at[j], partner)

    def w_done(j):
        rows = wt.at[pl.ds(dz(WSTEPS[j]) * NY, NY), 1 - c]
        arrived(rows, wd_r.at[j])

    def alone(run):
        pl.when(f >= 0)(run)

    def over_rows(first, size, body):
        def step(i, carry):
            body(pl.ds(pl.multiple_of(first + i * TILE, TILE), TILE))
            return carry

        lax.fori_loop(0, size // TILE, step, 0)

    def early(first, size):
        def body(rows):
            gate = eg[rows, :].astype(F32)
            eh[rows, :] = (gate * sigmoid(gate) * eu[rows, :].astype(F32)).astype(BF16)

        over_rows(first, size, body)

    def later(first, size):
        def body(rows):
            gate = lg[rows, :].astype(F32)
            lg[rows, :] = (gate * sigmoid(gate) * lu[rows, :].astype(F32)).astype(BF16)

        over_rows(first, size, body)

    def grad(k):
        cot_done(k)

        @alone
        def _():
            part = lax.dot_general(
                cot[:, columns(ZSTEPS[k])], eh[...], (((0,), (0,)), ((), ())), preferred_element_type=F32
            )
            gbuf[k] = part.astype(BF16).reshape(NY, NC, ROWS, part.shape[1])

        send(gbuf.at[k, :, 1 - c], precv.at[k], 6, gp_r.at[k], partner)

    def pair_done(k):
        arrived(precv.at[k], gp_r.at[k])

    def add_up(k, r, more):
        total = gbuf[k, dy(r), c].astype(F32) + precv[k, dy(r)].astype(F32)
        for d, i in more:
            total += zrecv[d, i].astype(F32)
        return total

    CHAIN = (
        ((0, -1), (0, 0), *((k, r) for k in (1, 3, 5) for r in (2, 1, -1, 0))),
        ((0, 2), (0, 1), (2, -1), (2, 2), (2, 1), (2, 0), (4, 2), (4, -1), (4, 1), (4, 0), (6, 2), (6, 1), (6, -1), (6, 0)),
    )

    def chain_before(d, k, r):
        nearer = ((1, 3, 5, 7), (2, 4, 6, 7))[d]
        before = (((0,) + nearer)[nearer.index(k)], r) if k in nearer else None
        if before not in CHAIN[d]:
            return []
        i = CHAIN[d].index(before)
        arrived(zrecv.at[d, i], gz_r.at[d, i])
        return [(d, i)]

    def chain(d, i):
        k, r = CHAIN[d][i]
        gbuf[k, dy(r), c] = add_up(k, r, chain_before(d, k, r)).astype(BF16)
        send(gbuf.at[k, dy(r), c], zrecv.at[d, i], 7, gz_r.at[d, i], at_z(SIDES[d][1]))

    def own_sum(i):
        r = (2, 1, -1)[i]
        gbuf[7, dy(r), c] = add_up(7, r, chain_before(0, 7, r) + chain_before(1, 7, r)).astype(BF16)
        send(gbuf.at[7, dy(r), c], yrecv.at[i], 8, gy_r.at[0], at_y(r))

    def grad_end():
        total = add_up(7, 0, chain_before(0, 7, 0) + chain_before(1, 7, 0))
        arrived(yrecv, gy_r.at[0])
        for i in range(3):
            total += yrecv[i].astype(F32)
        gsum[...] += total

    def partial(j):
        w_done(j)

        @alone
        def _():
            at = pl.ds(dz(WSTEPS[j]) * NY, NY)

            def product(cols, sign):
                rows = sign * wt[at, :, :, cols].reshape(WIDE, -1)
                return lax.dot_general(lg[:, cols], rows, (((1,), (1,)), ((), ())), preferred_element_type=F32)

            part = product(slice(0, KCUT), 1) - product(slice(KCUT, None), -1)
            pbuf[j] = part.astype(BF16).reshape(NX, xrows, WIDE)

        for d, s in SIDES:
            send(pbuf.at[j, dx(2), pl.ds(d * half, half)], pre.at[d, j], 9, mp_r.at[j], at_x(s))

    def partial_on(j):
        arrived(pre.at[:, 0], mp_r.at[j])
        for d, s in SIDES:
            rows = pl.ds(d * half, half)
            pbuf[j, dx(s), rows] = (pbuf[j, dx(s), rows].astype(F32) + pre[d, j].astype(F32)).astype(BF16)
            send(pbuf.at[j, dx(s)], full.at[d, j], 10, mf_r.at[j], at_x(s))

    def partial_end(j):
        arrived(full.at[:, 0], mf_r.at[j])
        total = pbuf[j, x].astype(F32) + full[0, j].astype(F32) + full[1, j].astype(F32)
        mixed[:, columns(WSTEPS[j])] = total.astype(BF16)

    def hidden(m, i):
        rows = pl.ds(m * xrows, xrows)
        cols = (slice(0, CUT), slice(CUT, None))[i]

        @alone
        def _():
            hc[:, cols] = jnp.dot(
                cot[rows, :], wt[:, :, :, cols].reshape(NZ * WIDE, -1), preferred_element_type=F32
            )


    def pointwise(m):
        def body(rows):
            sub = pl.ds(rows.start - m * xrows, TILE)
            gate, up, cotan = eg[rows, :].astype(F32), eu[rows, :].astype(F32), hc[sub, :]
            s = sigmoid(gate)
            scaled = cotan * s
            eg[rows, :] = (scaled * up * (1.0 + gate * (1.0 - s))).astype(BF16)
            eu[rows, :] = (scaled * gate).astype(BF16)

        over_rows(m * xrows, xrows, body)

    def begin():
        cot_direct(0)
        loads[3].wait()
        w_along_z(1, 0)
        w_along_z(1, 1)
        w_along_y(0)
        cot_direct(1)
        cot_direct(2)
        loads[0].wait()
        loads[1].wait()

    def later_loads():
        for copy in loads[4:]:
            copy.wait()

    quarter = tokens // 4
    tasks = {
        "B": begin,
        "e": lambda i: early(i * quarter, quarter),
        "c": loads[2].wait,
        "L": later_loads,
        "l": lambda i: later(i * quarter, quarter),
        "f": cot_forward,
        "g": grad,
        "d": pair_done,
        "z": w_z,
        "y": w_y,
        "k": w_core,
        "u": lambda i: chain(0, i),
        "v": lambda i: chain(1, i),
        "o": own_sum,
        "G": grad_end,
        "p": partial,
        "q": partial_on,
        "r": partial_end,
        "h": hidden,
        "w": pointwise,
    }
    for task in ORDER:
        tasks[task[0]](*(int(i) for i in task[1:].split("_") if i))
    for kind, like in enumerate(
        (full, pre, wt.at[pl.ds(0, 7), 0], wt.at[pl.ds(0, 16), 0], wt.at[pl.ds(0, 8), 0], precv, precv,
         wt.at[pl.ds(0, 28), 0], yrecv, pre, full)
    ):
        all_sent(kind, like)


def put_kernel(*refs):
    *refs, sem = refs
    half = len(refs) // 2
    copies = []
    for src, dst, parts in zip(refs[:half], refs[half:], PARTS):
        rows = src.shape[0] // parts
        for i in range(parts):
            at = pl.ds(i * rows, rows)
            copies.append(pltpu.make_async_copy(src.at[at], dst.at[at], sem.at[len(copies)]))
    for copy in copies:
        copy.start()
    for copy in copies:
        copy.wait()


def on_device(lg, lu, eg, eu, cot, weight, running):
    tokens, block = lg.shape
    xrows, width = cot.shape
    dma, vmem = pltpu.SemaphoreType.DMA, pltpu.VMEM
    mixed, gate_grad, up_grad, total = pl.pallas_call(
        kernel,
        out_shape=(
            vmem((xrows, width), BF16),
            vmem((tokens, block), BF16),
            vmem((tokens, block), BF16),
            vmem((ROWS, block), F32),
        ),
        in_specs=[pl.BlockSpec(memory_space=pl.ANY)] * 7,
        out_specs=[pl.BlockSpec(memory_space=vmem)] * 4,
        scratch_shapes=[
            *[vmem((tokens, block), BF16)] * 3,
            vmem((tokens, width), BF16),
            vmem((NZ * NY, NC, ROWS, block), BF16),
            vmem((NZ, NY, NC, ROWS, block), BF16),
            vmem((NZ, NY, ROWS, block), BF16),
            vmem((2, 14, ROWS, block), BF16),
            vmem((3, ROWS, block), BF16),
            vmem((NZ, NX, xrows, WIDE), BF16),
            vmem((2, NZ, xrows // 2, WIDE), BF16),
            vmem((2, NZ, xrows, WIDE), BF16),
            vmem((xrows, block), F32),
            dma((7,)),
            dma((11,)),
            dma((NZ,)),
            dma((NZ,)),
            dma((4, 2)),
            dma((NZ,)),
            dma((NZ,)),
            dma((NZ,)),
            dma((NZ,)),
            dma((2, 14)),
            dma((1,)),
            dma((NZ,)),
            dma((NZ,)),
        ],
        compiler_params=pltpu.CompilerParams(
            collective_id=0, has_side_effects=True, vmem_limit_bytes=52 * 1024 * 1024
        ),
        name="layer",
    )(lg, lu, eg, eu, cot, weight.T, running.T)
    results = (gate_grad, up_grad, mixed, total)
    gate_grad, up_grad, mixed, total = pl.pallas_call(
        put_kernel,
        out_shape=[jax.ShapeDtypeStruct(v.shape, v.dtype) for v in results],
        in_specs=[pl.BlockSpec(memory_space=vmem)] * 4,
        out_specs=[pl.BlockSpec(memory_space=pl.ANY)] * 4,
        scratch_shapes=[dma((sum(PARTS),))],
        compiler_params=pltpu.CompilerParams(vmem_limit_bytes=1 << 20),
        name="put",
    )(*results)
    return (mixed, gate_grad, up_grad, total.T)


def solution(mesh):
    tokens, hidden = P("fs", "tp"), P("tp", "fs")
    rows = P(("fs", "tp"), None)
    return jax.shard_map(
        on_device,
        mesh=mesh,
        in_specs=(tokens, tokens, tokens, tokens, rows, hidden, hidden),
        out_specs=(rows, tokens, tokens, hidden),
        check_vma=False,
    )
```

```python
import functools

import jax
import jax.numpy as jnp
from jax import lax
from jax.experimental import pallas as pl
from jax.experimental.pallas import tpu as pltpu
from jax.sharding import PartitionSpec as P

MESH = pl.DeviceIdType.MESH
F32, BF16 = jnp.float32, jnp.bfloat16
NX, NY, NZ, NC = 4, 4, 8, 2
ROWS = 32
WIDE = NY * NC * ROWS
TILE = 16
AHEAD = ((), (3,), (4,), (5,), (6,), (7,), (), ())
CUT = 1024
KCUT = 768
PARTS = (1, 1, 1, 1)


ORDER = (
    "B", "e0", "e1", "e2", "e3", "c", "L", "l0", "l1", "l2", "l3", "z1_0", "z1_1", "y0", "f0", "f1", "z2_0", "f2",
    "z2_1", "y1", "g0", "g1", "z3_0", "y2", "z3_1", "f3", "k0", "d0", "u0", "u1", "v0", "v1", "g2", "d1", "u2", "u3",
    "y3", "z4_0", "f4", "p0", "z4_1", "g3", "d2", "v2", "y4", "u4", "k1", "v3", "f5", "k2", "g4", "d3", "u5", "v4",
    "v5", "f6", "p1", "u6", "y5", "q0", "d4", "g5", "u7", "y6", "k3", "v6", "v7", "f7", "p2", "g6", "d5", "u8", "v8",
    "q1", "y7", "p3", "k4", "u9", "k5", "v9", "r0", "d6", "k6", "g7", "u10", "v10", "q2", "k7", "p4", "p5", "u11",
    "p6", "d7", "r1", "q3", "p7", "u12", "h0_0", "v11", "v12", "r2", "h0_1", "w0", "u13", "q4", "v13", "h1_0", "q5",
    "h1_1", "q6", "w1", "o0", "h2_0", "r3", "h2_1", "w2", "o1", "q7", "h3_0", "h3_1", "w3", "o2", "r4", "r5", "r6",
    "G", "r7",
)


def sigmoid(v):
    return 0.5 * jnp.tanh(0.5 * v) + 0.5


def kernel(
    lg_h, lu_h, eg_h, eu_h, cot_h, wt_h, running_h,
    mixed, eg, eu, gsum,
    lg, lu, eh, cot, wt, gbuf, precv, zrecv, yrecv, pbuf, pre, full, hc,
    load_sem, sent,
    cd_r, cf_r, wz_r, wy_r, wf_r, wd_r, gp_r, gz_r, gy_r, mp_r, mf_r,
):
    f, x = lax.axis_index("fs"), lax.axis_index("tp")
    c, y, z = lax.rem(f, NC), lax.rem(f // NC, NY), f // (NC * NY)
    xrows = cot_h.shape[0]
    half = xrows // 2
    hrow = ROWS // 2
    tokens = NX * xrows

    def dx(k):
        return lax.rem(x + (k + NX), NX)

    def dy(k):
        return lax.rem(y + (k + NY), NY)

    def dz(k):
        return lax.rem(z + (k + NZ), NZ)

    def at_x(k):
        return (f, dx(k))

    def at_y(k):
        return ((z * NY + dy(k)) * NC + c, x)

    def at_z(k):
        return ((dz(k) * NY + y) * NC + c, x)

    partner = ((z * NY + y) * NC + (1 - c), x)

    def send(src, dst, kind, rsem, to):
        pltpu.make_async_remote_copy(
            src_ref=src, dst_ref=dst, send_sem=sent.at[kind], recv_sem=rsem, device_id=to, device_id_type=MESH
        ).start()

    def arrived(dst, rsem):
        pltpu.make_async_remote_copy(
            src_ref=dst, dst_ref=dst, send_sem=sent.at[0], recv_sem=rsem, device_id=partner, device_id_type=MESH
        ).wait_recv()

    def all_sent(kind, like):
        pltpu.make_async_remote_copy(
            src_ref=like, dst_ref=like, send_sem=sent.at[kind], recv_sem=cd_r.at[0], device_id=partner, device_id_type=MESH
        ).wait_send()

    barrier = pltpu.get_barrier_semaphore()
    peers = [at_x(1), at_x(-1), at_y(1), at_y(-1), at_y(2), at_z(1), at_z(-1), partner]
    for peer in peers:
        pl.semaphore_signal(barrier, inc=1, device_id=peer, device_id_type=MESH)

    loads = [
        pltpu.make_async_copy(src, dst, load_sem.at[i])
        for i, (src, dst) in enumerate(
            [
                (eg_h, eg),
                (eu_h, eu),
                (cot_h, cot.at[pl.ds(pl.multiple_of(x * xrows, TILE), xrows)]),
                (wt_h, wt.at[z * NY + y, c]),
                (lg_h, lg),
                (lu_h, lu),
                (running_h, gsum),
            ]
        )
    ]
    for copy in loads:
        copy.start()

    pl.semaphore_wait(barrier, len(peers))

    SIDES = ((0, 1), (1, -1))
    ZSTEPS = (4, 3, -3, 2, -2, 1, -1, 0)
    WSTEPS = (0, -1, 1, -2, 2, -3, 3, 4)

    def columns(step):
        return pl.ds(pl.multiple_of(dz(step) * WIDE, WIDE), WIDE)

    def cot_rows(step, start=0, size=xrows):
        return pl.ds(pl.multiple_of(dx(step) * xrows + start, TILE), size)

    def cot_direct(k):
        cols = columns(ZSTEPS[k])
        for d, s in SIDES:
            send(cot_h.at[:, cols], cot.at[cot_rows(0), cols], 0, cd_r.at[k], at_x(s))

    def cot_forward(k):
        cols = columns(ZSTEPS[k])
        arrived(full.at[:, 0], cd_r.at[k])
        for d, s in SIDES:
            part = cot.at[cot_rows(-s, d * half, half), cols]
            send(part, part, 1, cf_r.at[k], at_x(s))
        for ahead in AHEAD[k]:
            cot_direct(ahead)

    def cot_done(k):
        arrived(pre.at[:, 0], cf_r.at[k])

    def w_block(zs, ys):
        return wt.at[dz(zs) * NY + dy(ys), c]

    def w_along_z(s, h):
        for d, step in SIDES:
            if s < 4 or d == h:
                part = w_block(-step * (s - 1), 0).at[pl.ds(h * hrow, hrow)]
                send(part, part, 2, wz_r.at[s - 1, h], at_z(step))

    def w_along_y(j):
        block = w_block(WSTEPS[j], 0)
        for d, step in SIDES:
            send(block, block, 3, wy_r.at[j], at_y(step))

    def w_z(s, h):
        arrived(wt.at[0, 0] if s < 4 else wt.at[0, 0, pl.ds(0, hrow)], wz_r.at[s - 1, h])
        if s < 4:
            w_along_z(s + 1, h)
        if h == 1:
            for j in (2 * s - 1, 2 * s) if s < 4 else (7,):
                w_along_y(j)

    def w_y(j):
        arrived(wt.at[0], wy_r.at[j])
        for d, step in SIDES:
            part = w_block(WSTEPS[j], -step).at[pl.ds(d * hrow, hrow)]
            send(part, part, 4, wf_r.at[j], at_y(step))

    def w_core(j):
        arrived(wt.at[0, 0], wf_r.at[j])
        rows = wt.at[pl.ds(dz(WSTEPS[j]) * NY, NY), c]
        send(rows, rows, 5, wd_r.at[j], partner)

    def w_done(j):
        rows = wt.at[pl.ds(dz(WSTEPS[j]) * NY, NY), 1 - c]
        arrived(rows, wd_r.at[j])

    def alone(run):
        pl.when(f >= 0)(run)

    def over_rows(first, size, body):
        def step(i, carry):
            body(pl.ds(pl.multiple_of(first + i * TILE, TILE), TILE))
            return carry

        lax.fori_loop(0, size // TILE, step, 0)

    def early(first, size):
        def body(rows):
            gate = eg[rows, :].astype(F32)
            eh[rows, :] = (gate * sigmoid(gate) * eu[rows, :].astype(F32)).astype(BF16)

        over_rows(first, size, body)

    def later(first, size):
        def body(rows):
            gate = lg[rows, :].astype(F32)
            lg[rows, :] = (gate * sigmoid(gate) * lu[rows, :].astype(F32)).astype(BF16)

        over_rows(first, size, body)

    def grad(k):
        cot_done(k)

        @alone
        def _():
            part = lax.dot_general(
                cot[:, columns(ZSTEPS[k])], eh[...], (((0,), (0,)), ((), ())), preferred_element_type=F32
            )
            gbuf[k] = part.astype(BF16).reshape(NY, NC, ROWS, part.shape[1])

        send(gbuf.at[k, :, 1 - c], precv.at[k], 6, gp_r.at[k], partner)

    def pair_done(k):
        arrived(precv.at[k], gp_r.at[k])

    def add_up(k, r, more):
        total = gbuf[k, dy(r), c].astype(F32) + precv[k, dy(r)].astype(F32)
        for d, i in more:
            total += zrecv[d, i].astype(F32)
        return total

    CHAIN = (
        ((0, -1), (0, 0), *((k, r) for k in (1, 3, 5) for r in (2, 1, -1, 0))),
        ((0, 2), (0, 1), (2, -1), (2, 2), (2, 1), (2, 0), (4, 2), (4, -1), (4, 1), (4, 0), (6, 2), (6, 1), (6, -1), (6, 0)),
    )

    def chain_sem(d, i):
        k, r = CHAIN[d][i]
        return gz_r.at[CHAIN[0].index((5, r)) if k == 6 else 14 * d + i]

    def chain_before(d, k, r):
        nearer = ((1, 3, 5, 7), (2, 4, 6, 7))[d]
        before = (((0,) + nearer)[nearer.index(k)], r) if k in nearer else None
        if before not in CHAIN[d]:
            return []
        i = CHAIN[d].index(before)
        if k < 7:
            arrived(zrecv.at[d, i], chain_sem(d, i))
        elif d == 0:
            arrived(wt.at[0], chain_sem(d, i))
        return [(d, i)]

    def chain(d, i):
        k, r = CHAIN[d][i]
        gbuf[k, dy(r), c] = add_up(k, r, chain_before(d, k, r)).astype(BF16)
        send(gbuf.at[k, dy(r), c], zrecv.at[d, i], 7, chain_sem(d, i), at_z(SIDES[d][1]))

    def own_sum(i):
        r = (2, 1, -1)[i]
        gbuf[7, dy(r), c] = add_up(7, r, chain_before(0, 7, r) + chain_before(1, 7, r)).astype(BF16)
        send(gbuf.at[7, dy(r), c], yrecv.at[i], 8, gy_r.at[0], at_y(r))

    def grad_end():
        total = add_up(7, 0, chain_before(0, 7, 0) + chain_before(1, 7, 0))
        arrived(yrecv, gy_r.at[0])
        for i in range(3):
            total += yrecv[i].astype(F32)
        gsum[...] += total

    def partial(j):
        w_done(j)

        @alone
        def _():
            at = pl.ds(dz(WSTEPS[j]) * NY, NY)

            def product(cols, sign):
                rows = sign * wt[at, :, :, cols].reshape(WIDE, -1)
                return lax.dot_general(lg[:, cols], rows, (((1,), (1,)), ((), ())), preferred_element_type=F32)

            part = product(slice(0, KCUT), 1) - product(slice(KCUT, None), -1)
            pbuf[j] = part.astype(BF16).reshape(NX, xrows, WIDE)

        for d, s in SIDES:
            send(pbuf.at[j, dx(2), pl.ds(d * half, half)], pre.at[d, j], 9, mp_r.at[j], at_x(s))

    def partial_on(j):
        arrived(pre.at[:, 0], mp_r.at[j])
        for d, s in SIDES:
            rows = pl.ds(d * half, half)
            pbuf[j, dx(s), rows] = (pbuf[j, dx(s), rows].astype(F32) + pre[d, j].astype(F32)).astype(BF16)
            send(pbuf.at[j, dx(s)], full.at[d, j], 10, mf_r.at[j], at_x(s))

    def partial_end(j):
        arrived(full.at[:, 0], mf_r.at[j])
        total = pbuf[j, x].astype(F32) + full[0, j].astype(F32) + full[1, j].astype(F32)
        mixed[:, columns(WSTEPS[j])] = total.astype(BF16)

    def hidden(m, i):
        rows = pl.ds(m * xrows, xrows)
        cols = (slice(0, CUT), slice(CUT, None))[i]

        @alone
        def _():
            hc[:, cols] = jnp.dot(
                cot[rows, :], wt[:, :, :, cols].reshape(NZ * WIDE, -1), preferred_element_type=F32
            )


    def pointwise(m):
        def body(rows):
            sub = pl.ds(rows.start - m * xrows, TILE)
            gate, up, cotan = eg[rows, :].astype(F32), eu[rows, :].astype(F32), hc[sub, :]
            s = sigmoid(gate)
            scaled = cotan * s
            eg[rows, :] = (scaled * up * (1.0 + gate * (1.0 - s))).astype(BF16)
            eu[rows, :] = (scaled * gate).astype(BF16)

        over_rows(m * xrows, xrows, body)

    def begin():
        cot_direct(0)
        loads[3].wait()
        w_along_z(1, 0)
        w_along_z(1, 1)
        w_along_y(0)
        cot_direct(1)
        cot_direct(2)
        loads[0].wait()
        loads[1].wait()

    def later_loads():
        for copy in loads[4:]:
            copy.wait()

    quarter = tokens // 4
    tasks = {
        "B": begin,
        "e": lambda i: early(i * quarter, quarter),
        "c": loads[2].wait,
        "L": later_loads,
        "l": lambda i: later(i * quarter, quarter),
        "f": cot_forward,
        "g": grad,
        "d": pair_done,
        "z": w_z,
        "y": w_y,
        "k": w_core,
        "u": lambda i: chain(0, i),
        "v": lambda i: chain(1, i),
        "o": own_sum,
        "G": grad_end,
        "p": partial,
        "q": partial_on,
        "r": partial_end,
        "h": hidden,
        "w": pointwise,
    }
    for task in ORDER:
        tasks[task[0]](*(int(i) for i in task[1:].split("_") if i))
    for kind, like in enumerate(
        (full, pre, wt.at[pl.ds(0, 7), 0], wt.at[pl.ds(0, 16), 0], wt.at[pl.ds(0, 8), 0], precv, precv,
         wt.at[pl.ds(0, 28), 0], yrecv, pre, full)
    ):
        all_sent(kind, like)


def put_kernel(*refs):
    *refs, sem = refs
    half = len(refs) // 2
    copies = []
    for src, dst, parts in zip(refs[:half], refs[half:], PARTS):
        rows = src.shape[0] // parts
        for i in range(parts):
            at = pl.ds(i * rows, rows)
            copies.append(pltpu.make_async_copy(src.at[at], dst.at[at], sem.at[len(copies)]))
    for i, copy in enumerate(copies):
        copy.start(priority=i % 2)
    for copy in copies:
        copy.wait()


def on_device(lg, lu, eg, eu, cot, weight, running):
    tokens, block = lg.shape
    xrows, width = cot.shape
    dma, vmem = pltpu.SemaphoreType.DMA, pltpu.VMEM
    mixed, gate_grad, up_grad, total = pl.pallas_call(
        kernel,
        out_shape=(
            vmem((xrows, width), BF16),
            vmem((tokens, block), BF16),
            vmem((tokens, block), BF16),
            vmem((ROWS, block), F32),
        ),
        in_specs=[pl.BlockSpec(memory_space=pl.ANY)] * 7,
        out_specs=[pl.BlockSpec(memory_space=vmem)] * 4,
        scratch_shapes=[
            *[vmem((tokens, block), BF16)] * 3,
            vmem((tokens, width), BF16),
            vmem((NZ * NY, NC, ROWS, block), BF16),
            vmem((NZ, NY, NC, ROWS, block), BF16),
            vmem((NZ, NY, ROWS, block), BF16),
            vmem((2, 14, ROWS, block), BF16),
            vmem((3, ROWS, block), BF16),
            vmem((NZ, NX, xrows, WIDE), BF16),
            vmem((2, NZ, xrows // 2, WIDE), BF16),
            vmem((2, NZ, xrows, WIDE), BF16),
            vmem((xrows, block), F32),
            dma((7,)),
            dma((11,)),
            dma((NZ,)),
            dma((NZ,)),
            dma((4, 2)),
            dma((NZ,)),
            dma((NZ,)),
            dma((NZ,)),
            dma((NZ,)),
            dma((24,)),
            dma((1,)),
            dma((NZ,)),
            dma((NZ,)),
        ],
        compiler_params=pltpu.CompilerParams(
            collective_id=0, has_side_effects=True, vmem_limit_bytes=52 * 1024 * 1024
        ),
        name="layer",
    )(lg, lu, eg, eu, cot, weight.T, running.T)
    results = (gate_grad, up_grad, mixed, total)
    gate_grad, up_grad, mixed, total = pl.pallas_call(
        put_kernel,
        out_shape=[jax.ShapeDtypeStruct(v.shape, v.dtype) for v in results],
        in_specs=[pl.BlockSpec(memory_space=vmem)] * 4,
        out_specs=[pl.BlockSpec(memory_space=pl.ANY)] * 4,
        scratch_shapes=[dma((sum(PARTS),))],
        compiler_params=pltpu.CompilerParams(vmem_limit_bytes=1 << 20),
        name="put",
    )(*results)
    return (mixed, gate_grad, up_grad, total.T)


def solution(mesh):
    tokens, hidden = P("fs", "tp"), P("tp", "fs")
    rows = P(("fs", "tp"), None)
    return jax.shard_map(
        on_device,
        mesh=mesh,
        in_specs=(tokens, tokens, tokens, tokens, rows, hidden, hidden),
        out_specs=(rows, tokens, tokens, hidden),
        check_vma=False,
    )
```
